32 devices in a mesh: fs: 4 (over z), rep: 4 (over y, x), tp: 2 (over core).
Axes of the slice: x: 2, y: 2, z: 4, core: 2. Of those that a mesh axis runs over, the one named last changes fastest.
Arguments:
- normed_in: bfloat16 [24576, 2048], P(('fs', 'rep')), may hold values from -6 to 6
- cotan_rec: bfloat16 [24576, 2048], P(('fs', 'rep'), 'tp'), may hold values from -0.0390625 to 0.0390625
- cotan_gate: bfloat16 [24576, 2048], P(('fs', 'rep'), 'tp'), may hold values from -0.0390625 to 0.0390625
- factor_rec: bfloat16 [2048, 512], P('fs'), may hold values from -0.125 to 0.125
- factor_gate: bfloat16 [2048, 512], P('fs'), may hold values from -0.125 to 0.125
- first_rec: float32 [512, 2048], P('fs', 'tp'), may hold values from -6 to 6
- first_gate: float32 [512, 2048], P('fs', 'tp'), may hold values from -6 to 6
- second_rec: float32 [512, 2048], P('fs', 'tp'), may hold values from 0.25 to 4
- second_gate: float32 [512, 2048], P('fs', 'tp'), may hold values from 0.25 to 4
- master_rec: float32 [2048, 2048], P('fs', 'tp'), may hold values from -0.125 to 0.125
- master_gate: float32 [2048, 2048], P('fs', 'tp'), may hold values from -0.125 to 0.125
Outputs:
- update_rec: float32 [2048, 2048], P('fs', 'tp')
- update_gate: float32 [2048, 2048], P('fs', 'tp')
- new_first_rec: float32 [512, 2048], P('fs', 'tp')
- new_first_gate: float32 [512, 2048], P('fs', 'tp')
- new_second_rec: float32 [512, 2048], P('fs', 'tp')
- new_second_gate: float32 [512, 2048], P('fs', 'tp')
- copy_rec: bfloat16 [2048, 2048], P(None, 'tp')
- copy_gate: bfloat16 [2048, 2048], P(None, 'tp')
The draws below stay inside these ranges and needn't reach their ends.
All inputs are finite; a program needn't handle non-finite values.
Results may differ from the reference program's by a relative error of at most 0.007.
Values may be sent and summed in bfloat16 or wider, within the bound.
No kernel may reach another device: no remote copies, remote signals or barrier semaphores. Data moves between devices by JAX's collectives and lax.ppermute only.
A program may use at most 128 MiB of HBM per device.

```python
import math
import jax
import jax.numpy as jnp
from jax import lax

D = 2048
DR = 2048
RANK = 512
TOKENS = 24576


def shard_levels(stream_key, shape, pieces, smallest, largest):
    loudness, own = 1.0, jax.random.fold_in(stream_key, 6)
    for axis_at, shards_of in pieces:
        heights = jnp.exp(jax.random.uniform(jax.random.fold_in(own, axis_at), (shards_of,), jnp.float32, smallest / len(pieces), largest / len(pieces)))
        loudness = loudness * jnp.repeat(heights, shape[axis_at] // shards_of).reshape([-1 if axis == axis_at else 1 for axis in range(len(shape))])
    return loudness


def centred(key, shape, scale, limit, cuts=(), dtype=jnp.bfloat16):
    factor_of = shard_levels(key, shape, cuts, -0.22, 0.18) if cuts else 1.0
    drawn = jax.random.normal(key, shape, jnp.float32) * scale * factor_of
    return jnp.minimum(jnp.maximum(drawn, -limit), limit).astype(dtype)


def setup_inputs(seed: int = 0) -> dict:
    key_of = jax.random.split(jax.random.key(seed), 12)
    return {
        "normed_in": centred(key_of[0], (TOKENS, D), 1.0, 6.0, ((0, 16),)),
        "cotan_rec": centred(key_of[1], (TOKENS, DR), (TOKENS ** -0.5), 0.0390625, ((0, 16), (1, 2))),
        "cotan_gate": centred(key_of[2], (TOKENS, DR), (TOKENS ** -0.5), 0.0390625, ((0, 16), (1, 2))),
        "factor_rec": centred(key_of[3], (D, RANK), D ** -0.5, 0.125, ((0, 4),)),
        "factor_gate": centred(key_of[4], (D, RANK), D ** -0.5, 0.125, ((0, 4),)),
        "first_rec": centred(key_of[5], (RANK, DR), 1.0, 6.0, ((0, 4), (1, 2)), jnp.float32),
        "first_gate": centred(key_of[6], (RANK, DR), 1.0, 6.0, ((0, 4), (1, 2)), jnp.float32),
        "second_rec": jnp.clip(jnp.exp(math.log(4.0) - 2.7725887 * jax.random.uniform(key_of[7], (RANK, DR), jnp.float32) ** shard_levels(key_of[7], (RANK, DR), ((0, 4), (1, 2)), -0.2, 0.2)), 0.25, 4.0),
        "second_gate": jnp.clip(jnp.exp(math.log(4.0) - 2.7725887 * jax.random.uniform(key_of[8], (RANK, DR), jnp.float32) ** shard_levels(key_of[8], (RANK, DR), ((0, 4), (1, 2)), -0.2, 0.2)), 0.25, 4.0),
        "master_rec": centred(key_of[9], (D, DR), D ** -0.5, 0.125, ((0, 4), (1, 2)), jnp.float32),
        "master_gate": centred(key_of[10], (D, DR), D ** -0.5, 0.125, ((0, 4), (1, 2)), jnp.float32),
    }


beta_first = 0.8
beta_second = 0.9
scale_floor = 0.25
step_rate = 0.01

def project_update(normed_in, cotan, factor, first, second, master):
    grad = lax.dot_general(normed_in, cotan, (((0,), (0,)), ((), ())), preferred_element_type=jnp.float32)
    factor_wide = factor.astype(jnp.float32)
    low = jnp.dot(factor_wide.T, grad, precision=lax.Precision.HIGHEST)
    new_first = beta_first * first + (1.0 - beta_first) * low
    new_second = beta_second * second + (1.0 - beta_second) * low * low
    direction = new_first / jnp.sqrt(new_second)
    scale = 1.0 / jnp.sqrt(jnp.mean(direction * direction) + scale_floor)
    update = jnp.dot(factor_wide, direction, precision=lax.Precision.HIGHEST) * scale
    copy = (master - step_rate * update).astype(jnp.bfloat16)
    return (update, new_first, new_second, copy)

def reference(normed_in, cotan_rec, cotan_gate, factor_rec, factor_gate, first_rec, first_gate, second_rec, second_gate, master_rec, master_gate):
    upd_rec, first_r, second_r, copy_rec = project_update(normed_in, cotan_rec, factor_rec, first_rec, second_rec, master_rec)
    upd_gate, first_g, second_g, copy_gate = project_update(normed_in, cotan_gate, factor_gate, first_gate, second_gate, master_gate)
    return (upd_rec, upd_gate, first_r, first_g, second_r, second_g, copy_rec, copy_gate)
```

```python
import functools

import jax
import jax.numpy as jnp
from jax import lax
from jax.experimental import pallas as pl
from jax.experimental.pallas import tpu as pltpu
from jax.sharding import PartitionSpec as P

beta_first = 0.8
beta_second = 0.9
scale_floor = 0.25
step_rate = 0.01


BF = jnp.bfloat16
F32 = jnp.float32
ANY = pl.BlockSpec(memory_space=pl.ANY)
VM = pl.BlockSpec(memory_space=pltpu.VMEM)
SM = pl.BlockSpec(memory_space=pltpu.SMEM)


def call(kernel, outs, ins, specs, out_specs, scratch=(), flops=1000000, name=None):
    return pl.pallas_call(
        kernel,
        out_shape=outs,
        in_specs=specs,
        out_specs=out_specs,
        scratch_shapes=list(scratch),
        compiler_params=pltpu.CompilerParams(vmem_limit_bytes=60 << 20),
        cost_estimate=pl.CostEstimate(flops=flops, bytes_accessed=1 << 20, transcendentals=0),
        name=name,
    )(*ins)


def sds(shape, dtype):
    return jax.ShapeDtypeStruct(shape, dtype)


def shift(x, k, n):
    return lax.ppermute(x, "fs", [(i, (i + k) % n) for i in range(n)])


def flip(x, axis, m, n):
    return lax.ppermute(x, axis, [(i, i ^ m) for i in range(n)])


def spread(parts, n):
    out = [[a] + [None] * (n - 1) for a in parts]
    if n == 4:
        hops = ((1, 2), (2, 1))
        for p, a in enumerate(parts):
            out[p][hops[p][0]] = flip(a, "rep", hops[p][0], n)
        for p, a in enumerate(parts):
            out[p][hops[p][1]] = flip(a, "rep", hops[p][1], n)
        for p, a in enumerate(parts):
            out[p][3] = flip(out[p][hops[p][0]], "rep", hops[p][1], n)
    else:
        for m in range(1, n):
            for p, a in enumerate(parts):
                out[p][m] = flip(a, "rep", m, n)
    return out


def low_kernel(sizes, order, s_ref, *refs):
    nf, nr, nt, D, K, N = sizes
    Dz, Kz = D // nf, K // nf
    De, R = Dz // (nr * nt), Kz // nr
    own, g, t = refs[:2], refs[2:4], refs[4 : 4 + 2 * nr * nt]
    f_out = refs[4 + 2 * nr * nt]
    keep = refs[5 + 2 * nr * nt : 7 + 2 * nr * nt]
    send = refs[7 + 2 * nr * nt : 9 + 2 * nr * nt]
    fv, gv, acc, sem_f, sem_g, sem_o = refs[9 + 2 * nr * nt :]
    z, r, c = s_ref[0], s_ref[1], s_ref[2]
    gd, fd = [], [[], []]
    for p in range(2):
        off = pl.multiple_of(z * Dz, Dz)
        d = pltpu.make_async_copy(own[p], fv.at[p, pl.ds(off, Dz)], sem_f.at[p, 0])
        d.start()
        fd[p].append(d)
        n = 1
        for m in range(nr):
            for h in range(nt):
                src = t[(p * nr + m) * nt + h]
                for k in range(1, nf):
                    zs = lax.rem(z + (nf - k), nf)
                    off = zs * Dz + lax.bitwise_xor(r, m) * (De * nt) + lax.bitwise_xor(c, h) * De
                    d = pltpu.make_async_copy(
                        src.at[k - 1], fv.at[p, pl.ds(pl.multiple_of(off, De), De)], sem_f.at[p, n]
                    )
                    d.start()
                    fd[p].append(d)
                    n += 1
        d = pltpu.make_async_copy(g[p], gv.at[p], sem_g.at[p])
        d.start()
        gd.append(d)
    od = []
    blk = D // 4
    for p in range(2):
        for d in fd[p]:
            d.wait()
        d = pltpu.make_async_copy(fv.at[p], f_out.at[p], sem_o.at[p])
        d.start()
        od.append(d)
        gd[p].wait()

        @pl.loop(0, 4)
        def _(b):
            rows = pl.ds(pl.multiple_of(b * blk, blk), blk)
            v = lax.dot_general(
                fv[p, rows, :], gv[p, rows, :], (((0,), (0,)), ((), ())), preferred_element_type=F32
            )

            @pl.when(b == 0)
            def _():
                acc[...] = v

            @pl.when(b > 0)
            def _():
                acc[...] += v

        bit = order[p][0]
        mine = lax.bitwise_and(lax.shift_right_logical(r, bit), 1)
        for zb in range(nf):
            for j in range(nr // 2):
                fixed = ((j >> bit) << (bit + 1)) | (j & ((1 << bit) - 1))
                base = zb * Kz + fixed * R
                k_off = base + mine * ((1 << bit) * R)
                s_off = base + (1 - mine) * ((1 << bit) * R)
                keep[p][zb, j] = acc[pl.ds(pl.multiple_of(k_off, R), R), :]
                send[p][zb, j] = acc[pl.ds(pl.multiple_of(s_off, R), R), :].astype(BF)
    for d in od:
        d.wait()


def half_kernel(sizes, bits, stage, s_ref, keep, recv, keep_out, send_out):
    nf, nr = sizes
    r = s_ref[1]
    bit = bits[stage]
    left = sorted(bits[stage:])
    pos = left.index(bit)
    mine = lax.bitwise_and(lax.shift_right_logical(r, bit), 1)
    for zb in range(nf):
        for j in range(keep_out.shape[1]):
            fixed = ((j >> pos) << (pos + 1)) | (j & ((1 << pos) - 1))
            k_at = fixed + mine * (1 << pos)
            s_at = fixed + (1 - mine) * (1 << pos)
            keep_out[zb, j] = keep[zb, k_at] + recv[zb, k_at].astype(F32)
            send_out[zb, j] = (keep[zb, s_at] + recv[zb, s_at].astype(F32)).astype(BF)


def split_kernel(nf, s_ref, *refs):
    keep, recv = refs[:2], refs[2:4]
    own, sends = refs[4], refs[5:]
    z = s_ref[0]
    for p in range(2):
        own[p] = keep[p][z, 0] + recv[p][z, 0].astype(F32)
        for k in range(1, nf):
            zb = lax.rem(z + k, nf)
            sends[k - 1][p] = (keep[p][zb, 0] + recv[p][zb, 0].astype(F32)).astype(BF)


def moment_kernel(nf, R, s_ref, *refs):
    own, recv = refs[0], refs[1:nf]
    first, second = refs[nf : nf + 2], refs[nf + 2 : nf + 4]
    direc, low_out = refs[nf + 4 :]
    rows = pl.ds(pl.multiple_of(s_ref[1] * R, R), R)
    for p in range(2):
        low = own[p]
        for v in recv:
            low = low + v[p].astype(F32)
        low_out[p] = low.astype(BF)
        new_first = beta_first * first[p][rows, :] + (1.0 - beta_first) * low
        new_second = beta_second * second[p][rows, :] + (1.0 - beta_second) * low * low
        direc[p] = (new_first / jnp.sqrt(new_second)).astype(BF)


def block_kernel(nf, s_ref, *refs):
    src, outs, part = refs[:nf], refs[nf : nf + 2], refs[nf + 2]
    z = s_ref[0]
    for p in range(2):
        for k in range(nf):
            outs[p][k] = src[k][p]
        total = None
        for zb in range(nf):
            v = outs[p][lax.rem(z + (nf - zb), nf)].astype(F32)
            v = v * v
            s = jnp.sum(v)
            total = s if total is None else total + s
        part[p] = jnp.full(part.shape[1:], total, F32)


def out_kernel(nr, R, s_ref, *refs):
    low = refs[:nr]
    first, second = refs[nr : nr + 2], refs[nr + 2 : nr + 4]
    nfirst, nsecond = refs[nr + 4 : nr + 6], refs[nr + 6 : nr + 8]
    r = s_ref[1]
    for p in range(2):
        for m in range(nr):
            rows = pl.ds(pl.multiple_of(lax.bitwise_xor(r, m) * R, R), R)
            v = low[m][p].astype(F32)
            nfirst[p][rows, :] = beta_first * first[p][rows, :] + (1.0 - beta_first) * v
            nsecond[p][rows, :] = beta_second * second[p][rows, :] + (1.0 - beta_second) * v * v


def final_kernel(sizes, way, s_ref, *refs):
    nf, nr, D, K, N, entries = sizes
    Dz, Kz = D // nf, K // nf
    R, Dh = Kz // nr, D // nf // 2
    it = iter(refs)
    tot = next(it)
    f_in = next(it)
    d_in = [[next(it) for _ in range(nr)] for _ in range(2)]
    m_own = [next(it) for _ in range(2)]
    e_in = [[next(it) for _ in range(2)] for _ in range(nf - 1)]
    x_in = [[next(it) for _ in range(2)] for _ in range(nf - 1)]
    upd = [next(it) for _ in range(2)]
    copy = [next(it) for _ in range(2)]
    fv, dv, mv, uv, cv, sem_f, sem_d, sem_m, sem_u, sem_c = it
    z, r = s_ref[0], s_ref[1]
    waits = [[], []]
    m_waits = [[], []]
    for p in range(2):
        n = 0
        for m in range(nr):
            for k in range(nf):
                off = lax.rem(z + (nf - k), nf) * Kz + lax.bitwise_xor(r, m) * R
                d = pltpu.make_async_copy(
                    d_in[p][m].at[k], dv.at[p, pl.ds(pl.multiple_of(off, R), R)], sem_d.at[p, n]
                )
                d.start()
                waits[p].append(d)
                n += 1
        d = pltpu.make_async_copy(f_in.at[p], fv.at[p], sem_f.at[p])
        d.start()
        waits[p].append(d)
        off = pl.multiple_of(z * Dz, Dz)
        d = pltpu.make_async_copy(m_own[p], mv.at[p, pl.ds(off, Dz)], sem_m.at[p, 0])
        d.start()
        m_waits[p].append(d)
        h = lax.bitwise_and(lax.shift_right_logical(r, way[p]), 1)
        for j in range(nf - 1):
            zb = s_ref[3 + j]
            for i, (src, hh) in enumerate(((e_in[j][p], h), (x_in[j][p], 1 - h))):
                off = pl.multiple_of(zb * Dz + hh * Dh, Dh)
                d = pltpu.make_async_copy(
                    src, mv.at[p, pl.ds(off, Dh)], sem_m.at[p, 1 + 2 * j + i]
                )
                d.start()
                m_waits[p].append(d)
    outs = []
    for p in range(2):
        scale = lax.rsqrt(tot[p, 0:1, 0:1] * (1.0 / entries) + scale_floor)
        for d in waits[p]:
            d.wait()
        for d in m_waits[p]:
            d.wait()
        rows_of = min(Dz, 256)

        @pl.loop(0, D // rows_of)
        def _(b):
            rows = pl.ds(pl.multiple_of(b * rows_of, rows_of), rows_of)
            v = jnp.dot(fv[p, rows, :], dv[p], preferred_element_type=F32) * scale
            cv[p, rows, :] = (mv[p, rows, :].astype(F32) - step_rate * v).astype(BF)
            at = b * rows_of - z * Dz

            @pl.when((at >= 0) & (at < Dz))
            def _():
                uv[p, pl.ds(pl.multiple_of(at, rows_of), rows_of), :] = v

        d = pltpu.make_async_copy(uv.at[p], upd[p], sem_u.at[p])
        d.start()
        outs.append(d)
        d = pltpu.make_async_copy(cv.at[p], copy[p], sem_c.at[p])
        d.start()
        outs.append(d)
    for d in outs:
        d.wait()


def arrival(nf):
    return [
        sorted((s for s in range(nf) if s != z), key=lambda s: (abs(s - z), (s < z) == (z < nf // 2)))
        for z in range(nf)
    ]


def body(nf, nr, nt, x, c_rec, c_gate, f_rec, f_gate, a_rec, a_gate, b_rec, b_gate, w_rec, w_gate):
    D, N = x.shape[1], c_rec.shape[1]
    Dz, K = f_rec.shape
    Kz = K // nf
    R, De, Dh = Kz // nr, Dz // (nr * nt), Dz // 2
    nb = nr.bit_length() - 1
    order = [[(p + i) % nb for i in range(nb)] for p in range(2)]
    way = [p % nb for p in range(2)]
    z, r, c = lax.axis_index("fs"), lax.axis_index("rep"), lax.axis_index("tp")
    table = arrival(nf)
    srcs = [sum(jnp.where(z == i, table[i][j], 0) for i in range(nf)) for j in range(nf - 1)]
    s = jnp.stack([z, r, c] + srcs).astype(jnp.int32)

    e = r * nt + c
    q = jnp.stack([lax.dynamic_slice_in_dim(f, e * De, De, 0) for f in (f_rec, f_gate)])
    got = [shift(q, k, nf) for k in range(1, nf)]
    t = spread([jnp.stack([g[p] for g in got]) for p in range(2)], nr)
    pieces = []
    for p in range(2):
        for m in range(nr):
            pieces.append(t[p][m])
            for h in range(1, nt):
                pieces.append(flip(t[p][m], "tp", h, nt))

    masters = [w.astype(BF) for w in (w_rec, w_gate)]
    halves = []
    for p in range(2):
        h = (r >> way[p]) & 1
        halves.append(lax.dynamic_slice_in_dim(masters[p], h * Dh, Dh, 0))
    right, left = {0: jnp.stack(halves)}, {}
    left[0] = right[0]
    for d in range(1, nf):
        right[d] = lax.ppermute(right[d - 1], "fs", [(i, i + 1) for i in range(d - 1, nf - 1)])
        left[d] = lax.ppermute(left[d - 1], "fs", [(i, i - 1) for i in range(1, nf - d + 1)])
    near, far = [], []
    for j in range(nf - 1):
        pick = None
        for i in range(nf):
            src = table[i][j]
            v = right[i - src] if src < i else left[src - i]
            pick = v if pick is None else jnp.where(z == i, v, pick)
        near.append([pick[p] for p in range(2)])
        far.append([flip(pick[p], "rep", 1 << way[p], nr) for p in range(2)])

    dims = (((0,), (0,)), ((), ()))
    g = [lax.dot_general(x, v, dims, preferred_element_type=F32).astype(BF) for v in (c_rec, c_gate)]
    n_sem = 1 + nr * nt * (nf - 1)
    f_full, keep0, keep1, send0, send1 = call(
        functools.partial(low_kernel, (nf, nr, nt, D, K, N), order),
        [sds((2, D, K), BF)]
        + [sds((nf, nr // 2, R, N), F32)] * 2
        + [sds((nf, nr // 2, R, N), BF)] * 2,
        [s, f_rec, f_gate, *g, *pieces],
        [SM] + [ANY] * (4 + len(pieces)),
        [ANY] + [VM] * 4,
        [
            pltpu.VMEM((2, D, K), BF),
            pltpu.VMEM((2, D, N), BF),
            pltpu.VMEM((K, N), F32),
            pltpu.SemaphoreType.DMA((2, n_sem)),
            pltpu.SemaphoreType.DMA((2,)),
            pltpu.SemaphoreType.DMA((2,)),
        ],
        flops=4 * D * K * N,
        name="low",
    )
    keep, send = [keep0, keep1], [send0, send1]
    recv = [flip(send[p], "rep", 1 << order[p][0], nr) for p in range(2)]
    for i in range(1, nb):
        width = nr >> (i + 1)
        for p in range(2):
            keep[p], send[p] = call(
                functools.partial(half_kernel, (nf, nr), order[p], i),
                [sds((nf, width, R, N), F32), sds((nf, width, R, N), BF)],
                [s, keep[p], recv[p]],
                [SM, VM, VM],
                [VM, VM],
                name="half",
            )
        recv = [flip(send[p], "rep", 1 << order[p][i], nr) for p in range(2)]
    own, *sends = call(
        functools.partial(split_kernel, nf),
        [sds((2, R, N), F32)] + [sds((2, R, N), BF)] * (nf - 1),
        [s, *keep, *recv],
        [SM] + [VM] * 4,
        [VM] * nf,
        name="split",
    )
    got = [shift(sends[k - 1], k, nf) for k in range(1, nf)]
    direc, low = call(
        functools.partial(moment_kernel, nf, R),
        [sds((2, R, N), BF)] * 2,
        [s, own, *got, a_rec, a_gate, b_rec, b_gate],
        [SM] + [VM] * (nf + 4),
        [VM] * 2,
        name="moments",
    )

    got = [shift(direc, k, nf) for k in range(1, nf)]
    d0, d1, part = call(
        functools.partial(block_kernel, nf),
        [sds((nf, R, N), BF)] * 2 + [sds((2, 8, 128), F32)],
        [s, direc, *got],
        [SM] + [VM] * nf,
        [VM] * 3,
        name="block",
    )
    dirs = spread([d0, d1], nr)
    total = part
    for h in range(nt.bit_length() - 1):
        total = total + flip(total, "tp", 1 << h, nt)
    for h in range(nb):
        total = total + flip(total, "rep", 1 << h, nr)

    lows = [low] + [flip(low, "rep", m, nr) for m in range(1, nr)]
    nf0, nf1, ns0, ns1 = call(
        functools.partial(out_kernel, nr, R),
        [sds((Kz, N), F32)] * 4,
        [s, *lows, a_rec, a_gate, b_rec, b_gate],
        [SM] + [VM] * (nr + 4),
        [VM] * 4,
        name="news",
    )

    flat = [v for p in range(2) for v in dirs[p]]
    flat += masters
    flat += [v for pair in near for v in pair] + [v for pair in far for v in pair]
    u0, u1, y0, y1 = call(
        functools.partial(final_kernel, (nf, nr, D, K, N, float(K * N * nt)), way),
        [sds((Dz, N), F32)] * 2 + [sds((D, N), BF)] * 2,
        [s, total, f_full, *flat],
        [SM, VM] + [ANY] * (1 + len(flat)),
        [ANY] * 4,
        [
            pltpu.VMEM((2, D, K), BF),
            pltpu.VMEM((2, K, N), BF),
            pltpu.VMEM((2, D, N), BF),
            pltpu.VMEM((2, Dz, N), F32),
            pltpu.VMEM((2, D, N), BF),
            pltpu.SemaphoreType.DMA((2,)),
            pltpu.SemaphoreType.DMA((2, nr * nf)),
            pltpu.SemaphoreType.DMA((2, 2 * nf - 1)),
            pltpu.SemaphoreType.DMA((2,)),
            pltpu.SemaphoreType.DMA((2,)),
        ],
        flops=4 * D * K * N,
        name="final",
    )
    return (u0, u1, nf0, nf1, ns0, ns1, y0, y1)


def solution(mesh):
    nf, nr, nt = mesh.shape["fs"], mesh.shape["rep"], mesh.shape["tp"]
    col = P(("fs", "rep"), "tp")
    both = P("fs", "tp")
    return jax.shard_map(
        functools.partial(body, nf, nr, nt),
        mesh=mesh,
        in_specs=(P(("fs", "rep"), None), col, col, P("fs", None), P("fs", None)) + (both,) * 6,
        out_specs=(both,) * 6 + (P(None, "tp"),) * 2,
        check_vma=False,
    )
```

```python
import functools

import jax
import jax.numpy as jnp
from jax import lax
from jax.experimental import pallas as pl
from jax.experimental.pallas import tpu as pltpu
from jax.sharding import PartitionSpec as P

beta_first = 0.8
beta_second = 0.9
scale_floor = 0.25
step_rate = 0.01


BF = jnp.bfloat16
F32 = jnp.float32
ANY = pl.BlockSpec(memory_space=pl.ANY)
VM = pl.BlockSpec(memory_space=pltpu.VMEM)
SM = pl.BlockSpec(memory_space=pltpu.SMEM)


def call(kernel, outs, ins, specs, out_specs, scratch=(), flops=1000000, name=None):
    return pl.pallas_call(
        kernel,
        out_shape=outs,
        in_specs=specs,
        out_specs=out_specs,
        scratch_shapes=list(scratch),
        compiler_params=pltpu.CompilerParams(vmem_limit_bytes=60 << 20),
        cost_estimate=pl.CostEstimate(flops=flops, bytes_accessed=1 << 20, transcendentals=0),
        name=name,
    )(*ins)


def sds(shape, dtype):
    return jax.ShapeDtypeStruct(shape, dtype)


def shift(x, k, n):
    return lax.ppermute(x, "fs", [(i, (i + k) % n) for i in range(n)])


def flip(x, axis, m, n):
    return lax.ppermute(x, axis, [(i, i ^ m) for i in range(n)])


def spread(parts, n):
    out = [[a] + [None] * (n - 1) for a in parts]
    if n == 4:
        hops = ((1, 2), (2, 1))
        for p, a in enumerate(parts):
            out[p][hops[p][0]] = flip(a, "rep", hops[p][0], n)
        for p, a in enumerate(parts):
            out[p][hops[p][1]] = flip(a, "rep", hops[p][1], n)
        for p, a in enumerate(parts):
            out[p][3] = flip(out[p][hops[p][0]], "rep", hops[p][1], n)
    else:
        for m in range(1, n):
            for p, a in enumerate(parts):
                out[p][m] = flip(a, "rep", m, n)
    return out


def gather_kernel(sizes, s_ref, *refs):
    nf, nr, nt, D, K = sizes
    Dz = D // nf
    De = Dz // (nr * nt)
    own, t, out, fv, sem, sem_o = refs[:2], refs[2:-4], refs[-4], refs[-3], refs[-2], refs[-1]
    z, r, c = s_ref[0], s_ref[1], s_ref[2]
    moves = [[], []]
    for p in range(2):
        off = pl.multiple_of(z * Dz, Dz)
        moves[p].append(pltpu.make_async_copy(own[p], fv.at[p, pl.ds(off, Dz)], sem.at[p, 0]))
        for m in range(nr):
            for h in range(nt):
                for k in range(1, nf):
                    zs = lax.rem(z + (nf - k), nf)
                    off = zs * Dz + lax.bitwise_xor(r, m) * (De * nt) + lax.bitwise_xor(c, h) * De
                    moves[p].append(
                        pltpu.make_async_copy(
                            t[m * nt + h].at[k - 1, p],
                            fv.at[p, pl.ds(pl.multiple_of(off, De), De)],
                            sem.at[p, len(moves[p])],
                        )
                    )
        for d in moves[p]:
            d.start()
    backs = []
    for p in range(2):
        for d in moves[p]:
            d.wait()
        d = pltpu.make_async_copy(fv.at[p], out.at[p], sem_o.at[p])
        d.start()
        backs.append(d)
    for d in backs:
        d.wait()


def part_kernel(sizes, bit, s_ref, low, keep, send):
    nf, nr, R = sizes
    mine = lax.bitwise_and(lax.shift_right_logical(s_ref[1], bit), 1)
    for zb in range(nf):
        for j in range(nr // 2):
            fixed = ((j >> bit) << (bit + 1)) | (j & ((1 << bit) - 1))
            base = zb * nr * R + fixed * R
            k_off = base + mine * ((1 << bit) * R)
            s_off = base + (1 - mine) * ((1 << bit) * R)
            keep[zb, j] = low[pl.ds(pl.multiple_of(k_off, R), R), :]
            send[zb, j] = low[pl.ds(pl.multiple_of(s_off, R), R), :].astype(BF)


def cast_kernel(Dh, way, s_ref, w0, w1, out):
    r = s_ref[1]
    for p, w in enumerate((w0, w1)):
        h = lax.bitwise_and(lax.shift_right_logical(r, way[p]), 1)
        out[p] = w[pl.ds(pl.multiple_of(h * Dh, Dh), Dh), :].astype(BF)


def choose_kernel(column, s_ref, *refs):
    ins, outs, sem = refs[:-3], refs[-3:-1], refs[-1]
    z = s_ref[0]
    for i, at in enumerate(column):

        @pl.when(z == i)
        def _():
            moves = [pltpu.make_async_copy(ins[at].at[p], outs[p], sem.at[p]) for p in range(2)]
            for d in moves:
                d.start()
            for d in moves:
                d.wait()


def half_kernel(sizes, bits, stage, s_ref, keep, recv, keep_out, send_out):
    nf, nr = sizes
    r = s_ref[1]
    bit = bits[stage]
    left = sorted(bits[stage:])
    pos = left.index(bit)
    mine = lax.bitwise_and(lax.shift_right_logical(r, bit), 1)
    for zb in range(nf):
        for j in range(keep_out.shape[1]):
            fixed = ((j >> pos) << (pos + 1)) | (j & ((1 << pos) - 1))
            k_at = fixed + mine * (1 << pos)
            s_at = fixed + (1 - mine) * (1 << pos)
            keep_out[zb, j] = keep[zb, k_at] + recv[zb, k_at].astype(F32)
            send_out[zb, j] = (keep[zb, s_at] + recv[zb, s_at].astype(F32)).astype(BF)


def split_kernel(nf, s_ref, *refs):
    keep, recv = refs[:2], refs[2:4]
    own, sends = refs[4], refs[5:]
    z = s_ref[0]
    for p in range(2):
        own[p] = keep[p][z, 0] + recv[p][z, 0].astype(F32)
        for k in range(1, nf):
            zb = lax.rem(z + k, nf)
            sends[k - 1][p] = (keep[p][zb, 0] + recv[p][zb, 0].astype(F32)).astype(BF)


def moment_kernel(nf, R, s_ref, *refs):
    own, recv = refs[0], refs[1:nf]
    first, second = refs[nf : nf + 2], refs[nf + 2 : nf + 4]
    direc, low_out = refs[nf + 4 :]
    rows = pl.ds(pl.multiple_of(s_ref[1] * R, R), R)
    for p in range(2):
        low = own[p]
        for v in recv:
            low = low + v[p].astype(F32)
        low_out[p] = low.astype(BF)
        new_first = beta_first * first[p][rows, :] + (1.0 - beta_first) * low
        new_second = beta_second * second[p][rows, :] + (1.0 - beta_second) * low * low
        direc[p] = (new_first / jnp.sqrt(new_second)).astype(BF)


def block_kernel(nf, s_ref, *refs):
    src, outs, part = refs[:nf], refs[nf : nf + 2], refs[nf + 2]
    z = s_ref[0]
    for p in range(2):
        for k in range(nf):
            outs[p][k] = src[k][p]
        total = None
        for zb in range(nf):
            v = outs[p][lax.rem(z + (nf - zb), nf)].astype(F32)
            v = v * v
            s = jnp.sum(v)
            total = s if total is None else total + s
        part[p] = jnp.full(part.shape[1:], total, F32)


def out_kernel(nr, R, s_ref, *refs):
    low = refs[:nr]
    first, second = refs[nr : nr + 2], refs[nr + 2 : nr + 4]
    nfirst, nsecond = refs[nr + 4 : nr + 6], refs[nr + 6 : nr + 8]
    r = s_ref[1]
    for p in range(2):
        for m in range(nr):
            rows = pl.ds(pl.multiple_of(lax.bitwise_xor(r, m) * R, R), R)
            v = low[m][p].astype(F32)
            nfirst[p][rows, :] = beta_first * first[p][rows, :] + (1.0 - beta_first) * v
            nsecond[p][rows, :] = beta_second * second[p][rows, :] + (1.0 - beta_second) * v * v


def final_kernel(sizes, way, s_ref, *refs):
    nf, nr, D, K, N, entries = sizes
    Dz, Kz = D // nf, K // nf
    R, Dh = Kz // nr, D // nf // 2
    it = iter(refs)
    tot = next(it)
    f_in = next(it)
    d_in = [[next(it) for _ in range(nr)] for _ in range(2)]
    w_in = [next(it) for _ in range(2)]
    e_in = [[next(it) for _ in range(2)] for _ in range(nf - 1)]
    x_in = [[next(it) for _ in range(2)] for _ in range(nf - 1)]
    upd = [next(it) for _ in range(2)]
    copy = [next(it) for _ in range(2)]
    fv, dv, mv, wv, uv, cv, sem_f, sem_d, sem_m, sem_w, sem_u, sem_c = it
    z, r = s_ref[0], s_ref[1]
    d_moves, f_moves, w_moves, m_moves = [[], []], [[], []], [], [[], []]
    spots = [z] + [s_ref[3 + j] for j in range(nf - 1)]
    rows_at = [pl.ds(pl.multiple_of(zb * Dz, Dz), Dz) for zb in spots]
    for p in range(2):
        for m in range(nr):
            for k in range(nf):
                off = lax.rem(z + (nf - k), nf) * Kz + lax.bitwise_xor(r, m) * R
                d = pltpu.make_async_copy(
                    d_in[p][m].at[k],
                    dv.at[p, pl.ds(pl.multiple_of(off, R), R)],
                    sem_d.at[p, m * nf + k],
                )
                d.start()
                d_moves[p].append(d)
        d = pltpu.make_async_copy(w_in[p], wv.at[p], sem_w.at[p])
        d.start()
        w_moves.append(d)
        h = lax.bitwise_and(lax.shift_right_logical(r, way[p]), 1)
        for j in range(nf):
            d = pltpu.make_async_copy(
                f_in.at[p, rows_at[j]], fv.at[p, rows_at[j]], sem_f.at[p, j]
            )
            d.start()
            f_moves[p].append(d)
            if j:
                pair = []
                for i, (src, hh) in enumerate(((e_in[j - 1][p], h), (x_in[j - 1][p], 1 - h))):
                    off = pl.multiple_of(spots[j] * Dz + hh * Dh, Dh)
                    d = pltpu.make_async_copy(
                        src, mv.at[p, pl.ds(off, Dh)], sem_m.at[p, 2 * (j - 1) + i]
                    )
                    d.start()
                    pair.append(d)
                m_moves[p].append(pair)
    outs = []
    step = min(Dz, 256)
    for p in range(2):
        scale = lax.rsqrt(tot[p, 0:1, 0:1] * (1.0 / entries) + scale_floor)
        for d in d_moves[p]:
            d.wait()
        for j in range(nf):
            f_moves[p][j].wait()
            if j:
                for d in m_moves[p][j - 1]:
                    d.wait()
            else:
                w_moves[p].wait()

            @pl.loop(0, Dz // step)
            def _(b):
                rows = pl.ds(pl.multiple_of(spots[j] * Dz + b * step, step), step)
                v = jnp.dot(fv[p, rows, :], dv[p], preferred_element_type=F32) * scale
                if j:
                    old = mv[p, rows, :]
                else:
                    mine = pl.ds(pl.multiple_of(b * step, step), step)
                    uv[p, mine, :] = v
                    old = wv[p, mine, :].astype(BF)
                cv[p, rows, :] = (old.astype(F32) - step_rate * v).astype(BF)

            if j == 0:
                d = pltpu.make_async_copy(uv.at[p], upd[p], sem_u.at[p])
                d.start()
                outs.append(d)
            d = pltpu.make_async_copy(cv.at[p, rows_at[j]], copy[p].at[rows_at[j]], sem_c.at[p, j])
            d.start()
            outs.append(d)
    for d in outs:
        d.wait()


def arrival(nf):
    return [
        sorted((s for s in range(nf) if s != z), key=lambda s: (abs(s - z), (s < z) == (z < nf // 2)))
        for z in range(nf)
    ]


def body(nf, nr, nt, x, c_rec, c_gate, f_rec, f_gate, a_rec, a_gate, b_rec, b_gate, w_rec, w_gate):
    D, N = x.shape[1], c_rec.shape[1]
    Dz, K = f_rec.shape
    Kz = K // nf
    R, De, Dh = Kz // nr, Dz // (nr * nt), Dz // 2
    nb = nr.bit_length() - 1
    order = [[(p + i) % nb for i in range(nb)] for p in range(2)]
    way = [p % nb for p in range(2)]
    z, r, c = lax.axis_index("fs"), lax.axis_index("rep"), lax.axis_index("tp")
    table = arrival(nf)
    srcs = [sum(jnp.where(z == i, table[i][j], 0) for i in range(nf)) for j in range(nf - 1)]
    s = jnp.stack([z, r, c] + srcs).astype(jnp.int32)

    dims = (((0,), (0,)), ((), ()))

    def outer(v):
        return lax.dot_general(x, v, dims, preferred_element_type=F32).astype(BF)

    e = r * nt + c
    q = jnp.stack([lax.dynamic_slice_in_dim(f, e * De, De, 0) for f in (f_rec, f_gate)])
    got = [shift(q, k, nf) for k in range(1, nf)]
    got, g0 = lax.optimization_barrier((got, outer(c_rec)))
    t = jnp.stack(got)
    t = [t] + [flip(t, "rep", m, nr) for m in range(1, nr)]
    t, g1 = lax.optimization_barrier((t, outer(c_gate)))
    g = [g0, g1]
    pieces = []
    for m in range(nr):
        pieces.append(t[m])
        for h in range(1, nt):
            pieces.append(flip(t[m], "tp", h, nt))
    n_sem = 1 + nr * nt * (nf - 1)
    f_full = call(
        functools.partial(gather_kernel, (nf, nr, nt, D, K)),
        sds((2, D, K), BF),
        [s, f_rec, f_gate, *pieces],
        [SM] + [ANY] * (2 + len(pieces)),
        ANY,
        [
            pltpu.VMEM((2, D, K), BF),
            pltpu.SemaphoreType.DMA((2, n_sem)),
            pltpu.SemaphoreType.DMA((2,)),
        ],
        name="factors",
    )

    halves = call(
        functools.partial(cast_kernel, Dh, way),
        sds((2, Dh, N), BF),
        [s, w_rec, w_gate],
        [SM, VM, VM],
        VM,
        name="cast",
    )
    right, left = {0: halves}, {0: halves}
    near, far = [], []
    for d in range(1, nf):
        right[d] = lax.ppermute(right[d - 1], "fs", [(i, i + 1) for i in range(d - 1, nf - 1)])
        left[d] = lax.ppermute(left[d - 1], "fs", [(i, i - 1) for i in range(1, nf - d + 1)])
    for j in range(nf - 1):
        ids = [(0, i - table[i][j]) if table[i][j] < i else (1, table[i][j] - i) for i in range(nf)]
        used = sorted(set(ids))
        pick = call(
            functools.partial(choose_kernel, [used.index(v) for v in ids]),
            [sds((Dh, N), BF)] * 2,
            [s] + [(right, left)[w][d] for w, d in used],
            [SM] + [ANY] * len(used),
            [ANY] * 2,
            [pltpu.SemaphoreType.DMA((2,))],
            name="choose",
        )
        near.append(pick)
        far.append([flip(pick[p], "rep", 1 << way[p], nr) for p in range(2)])

    keep, send = [None] * 2, [None] * 2
    for p in range(2):
        low = lax.dot_general(f_full[p], g[p], dims, preferred_element_type=F32)
        keep[p], send[p] = call(
            functools.partial(part_kernel, (nf, nr, R), order[p][0]),
            [sds((nf, nr // 2, R, N), F32), sds((nf, nr // 2, R, N), BF)],
            [s, low],
            [SM, VM],
            [VM, VM],
            name="part",
        )
    recv = [flip(send[p], "rep", 1 << order[p][0], nr) for p in range(2)]
    for i in range(1, nb):
        width = nr >> (i + 1)
        for p in range(2):
            keep[p], send[p] = call(
                functools.partial(half_kernel, (nf, nr), order[p], i),
                [sds((nf, width, R, N), F32), sds((nf, width, R, N), BF)],
                [s, keep[p], recv[p]],
                [SM, VM, VM],
                [VM, VM],
                name="half",
            )
        recv = [flip(send[p], "rep", 1 << order[p][i], nr) for p in range(2)]
    own, *sends = call(
        functools.partial(split_kernel, nf),
        [sds((2, R, N), F32)] + [sds((2, R, N), BF)] * (nf - 1),
        [s, *keep, *recv],
        [SM] + [VM] * 4,
        [VM] * nf,
        name="split",
    )
    got = [shift(sends[k - 1], k, nf) for k in range(1, nf)]
    direc, low = call(
        functools.partial(moment_kernel, nf, R),
        [sds((2, R, N), BF)] * 2,
        [s, own, *got, a_rec, a_gate, b_rec, b_gate],
        [SM] + [VM] * (nf + 4),
        [VM] * 2,
        name="moments",
    )

    got = [shift(direc, k, nf) for k in range(1, nf)]
    lows = [low] + [flip(low, "rep", m, nr) for m in range(1, nr)]
    got, lows = lax.optimization_barrier((got, lows))
    d0, d1, part = call(
        functools.partial(block_kernel, nf),
        [sds((nf, R, N), BF)] * 2 + [sds((2, 8, 128), F32)],
        [s, direc, *got],
        [SM] + [VM] * nf,
        [VM] * 3,
        name="block",
    )
    dirs = spread([d0, d1], nr)
    total = part
    for h in range(nt.bit_length() - 1):
        total = total + flip(total, "tp", 1 << h, nt)
    for h in range(nb):
        total = total + flip(total, "rep", 1 << h, nr)

    nf0, nf1, ns0, ns1 = call(
        functools.partial(out_kernel, nr, R),
        [sds((Kz, N), F32)] * 4,
        [s, *lows, a_rec, a_gate, b_rec, b_gate],
        [SM] + [VM] * (nr + 4),
        [VM] * 4,
        name="news",
    )

    flat = [v for p in range(2) for v in dirs[p]]
    flat += [w_rec, w_gate]
    flat += [v for pair in near for v in pair] + [v for pair in far for v in pair]
    u0, u1, y0, y1 = call(
        functools.partial(final_kernel, (nf, nr, D, K, N, float(K * N * nt)), way),
        [sds((Dz, N), F32)] * 2 + [sds((D, N), BF)] * 2,
        [s, total, f_full, *flat],
        [SM, VM] + [ANY] * (1 + len(flat)),
        [ANY] * 4,
        [
            pltpu.VMEM((2, D, K), BF),
            pltpu.VMEM((2, K, N), BF),
            pltpu.VMEM((2, D, N), BF),
            pltpu.VMEM((2, Dz, N), F32),
            pltpu.VMEM((2, Dz, N), F32),
            pltpu.VMEM((2, D, N), BF),
            pltpu.SemaphoreType.DMA((2, nf)),
            pltpu.SemaphoreType.DMA((2, nr * nf)),
            pltpu.SemaphoreType.DMA((2, 2 * nf)),
            pltpu.SemaphoreType.DMA((2,)),
            pltpu.SemaphoreType.DMA((2,)),
            pltpu.SemaphoreType.DMA((2, nf)),
        ],
        flops=4 * D * K * N,
        name="final",
    )
    return (u0, u1, nf0, nf1, ns0, ns1, y0, y1)


def solution(mesh):
    nf, nr, nt = mesh.shape["fs"], mesh.shape["rep"], mesh.shape["tp"]
    col = P(("fs", "rep"), "tp")
    both = P("fs", "tp")
    return jax.shard_map(
        functools.partial(body, nf, nr, nt),
        mesh=mesh,
        in_specs=(P(("fs", "rep"), None), col, col, P("fs", None), P("fs", None)) + (both,) * 6,
        out_specs=(both,) * 6 + (P(None, "tp"),) * 2,
        check_vma=False,
    )
```
